32 devices in a mesh: sp: 8 (over z, y), dp: 4 (over x, core).
Axes of the slice: x: 2, y: 2, z: 4, core: 2. Of those that a mesh axis runs over, the one named last changes fastest.
Arguments:
- tokens: bfloat16 [4, 1024, 2048], P('dp', 'sp'), may hold values from -6 to 6
- cotangent: bfloat16 [4, 1024, 2048], P('dp', 'sp'), may hold values from -6 to 6
- value_weight: bfloat16 [2048, 2048], P(('sp', 'dp')), may hold values from -0.125 to 0.125
- query_heads: bfloat16 [4, 1024, 16, 128], P('dp', None, 'sp'), may hold values from -8 to 8
- key_heads: bfloat16 [4, 1024, 16, 128], P('dp', None, 'sp'), may hold values from -8 to 8
- lambdas: float32 [16], P('sp'), may hold values from 0.3 to 0.8
Outputs:
- grad_query: bfloat16 [4, 1024, 16, 128], P('dp', None, 'sp')
- grad_key: bfloat16 [4, 1024, 16, 128], P('dp', None, 'sp')
- grad_tokens: bfloat16 [4, 1024, 2048], P('dp', 'sp')
- grad_value_weight: float32 [2048, 2048], P(('sp', 'dp'))
- grad_lambda: float32 [16], P('sp')
The draws below stay inside these ranges and needn't reach their ends.
All inputs are finite; a program needn't handle non-finite values.
Results may differ from the reference program's by a relative error of at most 0.0095.
Values may be sent and summed in bfloat16 or wider, within the bound.
No kernel may reach another device: no remote copies, remote signals or barrier semaphores. Data moves between devices by JAX's collectives and lax.ppermute only.
A program may use at most 192 MiB of HBM per device.

```python
import jax
import jax.numpy as jnp
from jax import lax

D = 2048
HEADS = 16
HEAD_DIM = 64
QBLOCK = 256
SEQS = 4
LENGTH = 1024
FEATURES = 2048


def pair_heads(key):
    array_shape = (SEQS, LENGTH, HEADS, 2 * HEAD_DIM)
    key_first = jax.random.fold_in(key, 11)
    key_second = jax.random.fold_in(key, 12)
    keys_part = jnp.clip(jax.random.normal(key_first, array_shape, jnp.float32) * 1.32, -8.0, 8.0)
    query_part = jnp.clip(jax.random.normal(key_second, array_shape, jnp.float32) * 1.32, -8.0, 8.0)
    return (query_part, keys_part)


def draw_query_heads(key, part):
    return pair_heads(key)[0].astype(jnp.bfloat16)


def draw_key_heads(key, part):
    return pair_heads(key)[1].astype(jnp.bfloat16)


def spiked(array, own_key, source, target, blocks, factor):
    def block_of(position):
        return (jnp.arange(array.shape[position]) // (array.shape[position] // blocks)).reshape((-1,) + (1,) * (array.ndim - 1 - position))

    first = jax.random.permutation(own_key, blocks)[block_of(target)]
    second = (block_of(target) + blocks // 2) % blocks
    return jnp.where((block_of(source) == first) | (block_of(source) == second), factor * array, array)


def block_levels(stream_key, shape, split, smallest, top_value):
    level, own = 1.0, jax.random.fold_in(stream_key, 6)
    for dim, blocks in split:
        steps = jnp.exp(jax.random.uniform(jax.random.fold_in(own, dim), (blocks,), jnp.float32, smallest / len(split), top_value / len(split)))
        level = level * jnp.repeat(steps, shape[dim] // blocks).reshape([-1 if axis == dim else 1 for axis in range(len(shape))])
    return level


def noise(own_key, shape, spread, limit, split=(), held_as=jnp.bfloat16):
    loudness = block_levels(own_key, shape, split, -0.22, 0.18) if split else 1.0
    values = jax.random.normal(own_key, shape, jnp.float32) * spread * loudness
    return jnp.minimum(jnp.maximum(values, -limit), limit).astype(held_as)


def bell_draw_with(rng, dims, deviation, reach, cuts, heavy, kind=jnp.bfloat16):
    drawn = deviation * jax.random.normal(rng, dims, jnp.float32)
    if cuts:
        drawn = drawn * block_levels(rng, dims, cuts, -0.22, 0.18)
    return jnp.clip(spiked(drawn, jax.random.fold_in(rng, 3), *heavy), -reach, reach).astype(kind)


def setup_inputs(seed: int = 0) -> dict:
    key_of = jax.random.split(jax.random.key(seed), 7)
    tokens = bell_draw_with(key_of[0], (SEQS, LENGTH, D), 1.0, 6.0, ((0, 4), (1, 8)), (1, 2, 8, 2.0))
    cotangent = noise(key_of[1], (SEQS, LENGTH, FEATURES), 1.0, 6.0, ((0, 4), (1, 8)))
    value_weight = noise(key_of[2], (D, FEATURES), D ** -0.5, 0.125, ((0, 32),))
    query_heads = draw_query_heads(jax.random.fold_in(key_of[6], 71), 0)
    key_heads = draw_key_heads(jax.random.fold_in(key_of[6], 71), 0)
    lambdas = jnp.clip(0.3 + 0.5 * jax.random.uniform(key_of[5], (HEADS,), jnp.float32) ** block_levels(key_of[5], (HEADS,), ((0, 8),), -0.2, 0.2), 0.3, 0.8)
    return {"tokens": tokens, "cotangent": cotangent, "value_weight": value_weight, "query_heads": query_heads, "key_heads": key_heads, "lambdas": lambdas}


EPS = 1e-06
NEGATIVE = -1e+30

def head_backward(queries, keys_in, values_in, cotangent, lambdas, block_rows):
    seq_length = queries.shape[0]
    head_count = queries.shape[1]
    head_width = queries.shape[3]
    scaling = head_width ** (-0.5)
    blocks_count = seq_length // block_rows
    positions = jnp.arange(seq_length, dtype=jnp.int32)
    keys_wide = keys_in.astype(jnp.float32)
    values_wide = values_in.astype(jnp.float32)
    lambda_col = lambdas[:, None, None]

    def block_step(totals, block_index):
        grad_key_sum, grad_value_sum, grad_lambda_sum = totals
        offset = (block_index * block_rows).astype(jnp.int32)
        query_block = lax.dynamic_slice_in_dim(queries, offset, block_rows, 0).astype(jnp.float32)
        cotan_block = lax.dynamic_slice_in_dim(cotangent, offset, block_rows, 0).astype(jnp.float32)
        scores = jnp.einsum('qhcd,khcd->hcqk', query_block, keys_wide) * scaling
        rows_pos = offset + jnp.arange(block_rows, dtype=jnp.int32)
        allowed = rows_pos[:, None] >= positions[None, :]
        scores = jnp.where(allowed, scores, NEGATIVE)
        highest = lax.optimization_barrier(jnp.max(scores, axis=-1, keepdims=True))
        exponent = jnp.exp(scores - highest)
        softmaxes = exponent / lax.optimization_barrier(jnp.sum(exponent, axis=-1, keepdims=True))
        weights = (softmaxes[:, 0] - lambda_col * softmaxes[:, 1]).astype(jnp.bfloat16)
        weights_wide = weights.astype(jnp.float32)
        mixed_out = jnp.einsum('hqk,khd->qhd', weights_wide, values_wide)
        inverse = lax.rsqrt(lax.optimization_barrier(jnp.mean(mixed_out * mixed_out, axis=-1, keepdims=True)) + EPS)
        normed = mixed_out * inverse
        grad_mixed = (inverse * (cotan_block - normed * lax.optimization_barrier(jnp.mean(cotan_block * normed, axis=-1, keepdims=True)))).astype(jnp.bfloat16)
        grad_mixed_wide = grad_mixed.astype(jnp.float32)
        grad_weights = jnp.einsum('qhd,khd->hqk', grad_mixed_wide, values_wide)
        grad_value_sum = grad_value_sum + jnp.einsum('hqk,qhd->khd', weights_wide, grad_mixed_wide)
        grad_lambda_sum = grad_lambda_sum - lax.optimization_barrier(jnp.sum(grad_weights * softmaxes[:, 1], axis=(1, 2)))
        first_grad = softmaxes[:, 0] * (grad_weights - lax.optimization_barrier(jnp.sum(grad_weights * softmaxes[:, 0], axis=-1, keepdims=True)))
        second_grad = -lambda_col * softmaxes[:, 1] * (grad_weights - lax.optimization_barrier(jnp.sum(grad_weights * softmaxes[:, 1], axis=-1, keepdims=True)))
        grad_scores = (jnp.stack([first_grad, second_grad], axis=1) * scaling).astype(jnp.bfloat16)
        grad_scores_wide = grad_scores.astype(jnp.float32)
        grad_query_block = jnp.einsum('hcqk,khcd->qhcd', grad_scores_wide, keys_wide).astype(jnp.bfloat16)
        grad_key_sum = grad_key_sum + jnp.einsum('hcqk,qhcd->khcd', grad_scores_wide, query_block)
        return ((grad_key_sum, grad_value_sum, grad_lambda_sum), grad_query_block)
    initial = (jnp.zeros(keys_in.shape, jnp.float32), jnp.zeros(values_in.shape, jnp.float32), jnp.zeros((head_count,), jnp.float32))
    totals, query_blocks = lax.scan(block_step, initial, jnp.arange(blocks_count, dtype=jnp.int32))
    grad_query = query_blocks.reshape(queries.shape)
    return (grad_query, totals[0].astype(jnp.bfloat16), totals[1].astype(jnp.bfloat16), totals[2])

def reference(tokens, cotangent, value_weight, query_heads, key_heads, lambdas):
    seq_count = tokens.shape[0]
    seq_length = tokens.shape[1]
    feature_count = value_weight.shape[1]
    flat_tokens = tokens.reshape(seq_count * seq_length, D)
    values_flat = jnp.dot(flat_tokens, value_weight, preferred_element_type=jnp.float32).astype(jnp.bfloat16)
    values_heads = values_flat.reshape(seq_count, seq_length, HEADS, 2 * HEAD_DIM)
    cotan_heads = cotangent.reshape(seq_count, seq_length, HEADS, 2 * HEAD_DIM)
    queries = query_heads.reshape(seq_count, seq_length, HEADS, 2, HEAD_DIM)
    keys_in = key_heads.reshape(seq_count, seq_length, HEADS, 2, HEAD_DIM)

    def one_sequence(items):
        return head_backward(items[0], items[1], items[2], items[3], lambdas, QBLOCK)
    grad_query, grad_key, grad_value, grad_lambda = lax.map(one_sequence, (queries, keys_in, values_heads, cotan_heads))
    grad_lambda = lax.optimization_barrier(jnp.sum(grad_lambda, axis=0))
    grad_flat = grad_value.reshape(seq_count * seq_length, feature_count)
    grad_tokens = jnp.dot(grad_flat, value_weight.T, preferred_element_type=jnp.float32).astype(jnp.bfloat16)
    grad_weight = jnp.dot(flat_tokens.T, grad_flat, preferred_element_type=jnp.float32)
    return (grad_query.reshape(query_heads.shape), grad_key.reshape(key_heads.shape), grad_tokens.reshape(tokens.shape), grad_weight, grad_lambda)
```

```python
import jax
import jax.numpy as jnp
from jax import lax
from jax.experimental import pallas as pl
from jax.experimental.pallas import tpu as pltpu
from jax.sharding import Mesh
from jax.sharding import PartitionSpec as P

QBLOCK = 256


EPS = 1e-06
NEGATIVE = -1e30

NT = (((1,), (1,)), ((), ()))


def dot(a, b):
    return jnp.dot(a, b, preferred_element_type=jnp.float32)


def dot_nt(a, b):
    return lax.dot_general(a, b, NT, preferred_element_type=jnp.float32)


def attention_kernel(
    lambda_ref, q_ref, k_ref, v_ref, g_ref, gq_ref, gk_ref, gv_ref, gl_ref, dk_acc, dv_acc
):
    seq_length, width = q_ref.shape
    half = width // 2
    scaling = half ** (-0.5)
    rows = min(QBLOCK, seq_length)
    blocks = seq_length // rows
    lam = lambda_ref[pl.program_id(0)]
    first = lax.broadcasted_iota(jnp.int32, (rows, width), 1) < half
    allowed = lax.broadcasted_iota(jnp.int32, (rows, rows), 0) >= lax.broadcasted_iota(
        jnp.int32, (rows, rows), 1
    )
    grad_lambda = jnp.zeros((rows, 1), jnp.float32)

    def softmax(scores, lo):
        diagonal = jnp.where(allowed, scores[:, lo:], NEGATIVE)
        scores = jnp.concatenate([scores[:, :lo], diagonal], axis=1) if lo else diagonal
        exponent = jnp.exp(scores - jnp.max(scores, axis=-1, keepdims=True))
        return exponent * (1.0 / jnp.sum(exponent, axis=-1, keepdims=True))

    for block in reversed(range(blocks)):
        lo = block * rows
        hi = lo + rows
        q = q_ref[lo:hi, :].astype(jnp.float32) * scaling
        zero = jnp.zeros_like(q)
        stacked = jnp.concatenate([jnp.where(first, q, zero), jnp.where(first, zero, q)], axis=0)
        keys = k_ref[:hi, :]
        values = v_ref[:hi, :]
        scores = dot_nt(stacked.astype(jnp.bfloat16), keys)
        p1 = softmax(scores[:rows], lo)
        p2 = softmax(scores[rows:], lo)
        w2 = lam * p2
        weights = (p1 - w2).astype(jnp.bfloat16)
        mixed = dot(weights, values)
        inverse = lax.rsqrt(jnp.mean(mixed * mixed, axis=-1, keepdims=True) + EPS)
        normed = mixed * inverse
        cotan = g_ref[lo:hi, :].astype(jnp.float32)
        grad_mixed = inverse * (cotan - normed * jnp.mean(cotan * normed, axis=-1, keepdims=True))
        grad_weights = dot_nt(grad_mixed.astype(jnp.bfloat16), values)
        value_part = dot(grad_mixed.T.astype(jnp.bfloat16), weights)
        t1 = jnp.sum(grad_weights * p1, axis=-1, keepdims=True)
        t2 = jnp.sum(grad_weights * p2, axis=-1, keepdims=True)
        grad_lambda = grad_lambda - t2
        ds = jnp.concatenate(
            [
                (p1 * (grad_weights - t1)).astype(jnp.bfloat16),
                (w2 * (t2 - grad_weights)).astype(jnp.bfloat16),
            ],
            axis=0,
        )
        dq = dot(ds, keys)
        gq_ref[lo:hi, :] = (jnp.where(first, dq[:rows], dq[rows:]) * scaling).astype(jnp.bfloat16)
        key_part = dot(stacked.T.astype(jnp.bfloat16), ds)
        if block == blocks - 1:
            dv_acc[...] = value_part
            dk_acc[...] = key_part
        else:
            dv_acc[:, :hi] += value_part
            dk_acc[:, :hi] += key_part
    gk_ref[...] = dk_acc[...].T.astype(jnp.bfloat16)
    gv_ref[...] = dv_acc[...].T.astype(jnp.bfloat16)
    gl_ref[...] = jnp.broadcast_to(jnp.sum(grad_lambda).reshape(1, 1, 1), gl_ref.shape)


def head_backward(queries, keys, values, cotangent, lambdas):
    seq_length = queries.shape[0]
    heads = lambdas.shape[0]
    width = queries.shape[1] // heads
    block = pl.BlockSpec((seq_length, width), lambda h: (0, h))
    grads = jax.ShapeDtypeStruct(queries.shape, jnp.bfloat16)
    gq, gk, gv, gl = pl.pallas_call(
        attention_kernel,
        grid=(heads,),
        in_specs=[pl.BlockSpec(memory_space=pltpu.SMEM), block, block, block, block],
        out_specs=[block, block, block, pl.BlockSpec((1, 8, 128), lambda h: (h, 0, 0))],
        out_shape=[grads, grads, grads, jax.ShapeDtypeStruct((heads, 8, 128), jnp.float32)],
        scratch_shapes=[
            pltpu.VMEM((width, seq_length), jnp.float32),
            pltpu.VMEM((width, seq_length), jnp.float32),
        ],
        compiler_params=pltpu.CompilerParams(dimension_semantics=("arbitrary",)),
        cost_estimate=pl.CostEstimate(
            flops=20 * heads * seq_length * seq_length * width,
            bytes_accessed=14 * heads * seq_length * width,
            transcendentals=2 * heads * seq_length * seq_length,
        ),
    )(lambdas, queries, keys, values, cotangent)
    return gq, gk, gv, gl[:, 0, 0]


def partners(size):
    if size & (size - 1) == 0:
        return [[i ^ k for i in range(size)] for k in range(1, size)]
    return [[(i + k) % size for i in range(size)] for k in range(1, size)]


def source_index(target, axis):
    source = [0] * len(target)
    for sender, receiver in enumerate(target):
        source[receiver] = sender
    return jnp.array(source, jnp.int32)[lax.axis_index(axis)]


def send(x, axis, target):
    return lax.ppermute(x, axis, list(enumerate(target)))


def gathered(x, axis):
    pieces = [(lax.axis_index(axis), x)]
    for target in partners(lax.axis_size(axis)):
        pieces.append((source_index(target, axis), send(x, axis, target)))
    return pieces


def scattered_sum(x, axis):
    mine = lax.axis_index(axis)
    total = lax.dynamic_index_in_dim(x, mine, 0, keepdims=False).astype(jnp.float32)
    for target in partners(lax.axis_size(axis)):
        block = lax.dynamic_index_in_dim(
            x, jnp.array(target, jnp.int32)[mine], 0, keepdims=False
        )
        total = total + send(block, axis, target).astype(jnp.float32)
    return total


def body(tokens, cotangent, value_weight, query_heads, key_heads, lambdas):
    groups = lax.axis_size("g")
    pair = lax.axis_size("p")
    chips = lax.axis_size("x")
    cores = lax.axis_size("c")
    dp_count = chips * cores
    local_tokens = tokens[0]
    block_tokens, model_width = local_tokens.shape
    row_count, features = value_weight.shape
    head_features = features // (pair * groups)
    group_features = pair * head_features
    seq_length = query_heads.shape[1]

    some_tokens = jnp.zeros((groups, block_tokens, model_width), tokens.dtype)
    for index, piece in gathered(local_tokens, "g"):
        some_tokens = lax.dynamic_update_slice(some_tokens, piece[None], (index, 0, 0))
    some_tokens = some_tokens.reshape(groups * block_tokens, model_width)

    mine = lax.all_to_all(
        value_weight.reshape(row_count, pair, groups, head_features)
        .transpose(2, 0, 1, 3)
        .reshape(groups, row_count, group_features),
        "g",
        split_axis=0,
        concat_axis=0,
        tiled=True,
    )
    columns = jnp.zeros((pair, groups, chips, cores, row_count, group_features), mine.dtype)
    for p_index, p_piece in gathered(mine, "p"):
        for x_index, x_piece in gathered(p_piece, "x"):
            for c_index, piece in gathered(x_piece, "c"):
                columns = lax.dynamic_update_slice(
                    columns, piece[None, :, None, None], (p_index, 0, x_index, c_index, 0, 0)
                )
    columns = columns.reshape(model_width, group_features)

    cotan_heads = lax.all_to_all(
        cotangent[0], ("p", "g"), split_axis=1, concat_axis=0, tiled=True
    )
    some_values = dot(some_tokens, columns).astype(jnp.bfloat16)
    value_heads = lax.all_to_all(some_values, "p", split_axis=1, concat_axis=0, tiled=True)
    flat = (seq_length, head_features)
    gq, gk, gv, grad_lambda = head_backward(
        query_heads.reshape(flat), key_heads.reshape(flat), value_heads, cotan_heads, lambdas
    )
    lambda_grad = grad_lambda
    for x_target in [list(range(chips))] + partners(chips):
        for c_target in [list(range(cores))] + partners(cores):
            target = [x * cores + c for x in x_target for c in c_target]
            if target != list(range(dp_count)):
                lambda_grad = lambda_grad + send(grad_lambda, ("x", "c"), target)

    grad_values = lax.all_to_all(gv, "p", split_axis=0, concat_axis=1, tiled=True)

    term = lax.dot_general(
        some_tokens, grad_values, (((0,), (0,)), ((), ())), preferred_element_type=jnp.float32
    ).astype(jnp.bfloat16)
    term = term.reshape(pair, groups, chips, cores, row_count, group_features)
    term = scattered_sum(term.transpose(3, 2, 0, 1, 4, 5), "c").astype(jnp.bfloat16)
    term = scattered_sum(term, "x").astype(jnp.bfloat16)
    term = scattered_sum(term, "p").astype(jnp.bfloat16)

    parts = dot_nt(grad_values, columns).astype(jnp.bfloat16)
    parts = lax.all_to_all(
        parts.reshape(groups, block_tokens, model_width), "g", split_axis=0, concat_axis=0, tiled=True
    )
    grad_tokens = jnp.sum(parts.astype(jnp.float32), axis=0).astype(jnp.bfloat16)

    grad_weight = lax.all_to_all(term, "g", split_axis=0, concat_axis=0, tiled=True)
    grad_weight = grad_weight.reshape(groups, row_count, pair, head_features)
    grad_weight = grad_weight.transpose(1, 2, 0, 3).reshape(row_count, features)
    return (
        gq.reshape(query_heads.shape),
        gk.reshape(key_heads.shape),
        grad_tokens[None],
        grad_weight.astype(jnp.float32),
        lambda_grad,
    )


def solution(mesh):
    sp_count = mesh.shape["sp"]
    dp_count = mesh.shape["dp"]
    pair = 2 if sp_count % 2 == 0 else 1
    cores = 2 if dp_count % 2 == 0 else 1
    inner = Mesh(
        mesh.devices.reshape(pair, sp_count // pair, dp_count // cores, cores),
        ("p", "g", "x", "c"),
    )
    sp = ("p", "g")
    dp = ("x", "c")
    token_spec = P(dp, sp, None)
    head_spec = P(dp, None, sp, None)
    weight_spec = P(sp + dp, None)
    return jax.shard_map(
        body,
        mesh=inner,
        in_specs=(token_spec, token_spec, weight_spec, head_spec, head_spec, P(sp)),
        out_specs=(head_spec, head_spec, token_spec, weight_spec, P(sp)),
        check_vma=False,
    )
```

```python
import functools

import jax
import jax.numpy as jnp
from jax import lax
from jax.experimental import pallas as pl
from jax.experimental.pallas import tpu as pltpu
from jax.sharding import Mesh
from jax.sharding import PartitionSpec as P


QBLOCK = 256


EPS = 1e-06
NEGATIVE = -1e30

NT = (((1,), (1,)), ((), ()))


def dot(a, b):
    return jnp.dot(a, b, preferred_element_type=jnp.float32)


def dot_nt(a, b):
    return lax.dot_general(a, b, NT, preferred_element_type=jnp.float32)


def attention_kernel(
    lambda_ref,
    place_ref,
    q_ref,
    k_ref,
    own_ref,
    other_ref,
    g_ref,
    gq_ref,
    gk_ref,
    gown_ref,
    gother_ref,
    gl_ref,
    dk_acc,
    dv_acc,
    v_ref,
    *,
    head,
):
    seq_length, width = q_ref.shape
    span = own_ref.shape[0]
    own_rows = pl.ds(pl.multiple_of(place_ref[0] * span, span), span)
    other_rows = pl.ds(pl.multiple_of((1 - place_ref[0]) * span, span), span)
    v_ref[own_rows, :] = own_ref[...]
    v_ref[other_rows, :] = other_ref[...]
    half = width // 2
    scaling = half ** (-0.5)
    rows = min(QBLOCK, seq_length)
    blocks = seq_length // rows
    lam = lambda_ref[head]
    first = lax.broadcasted_iota(jnp.int32, (rows, width), 1) < half
    allowed = lax.broadcasted_iota(jnp.int32, (rows, rows), 0) >= lax.broadcasted_iota(
        jnp.int32, (rows, rows), 1
    )
    grad_lambda = jnp.zeros((rows, 1), jnp.float32)

    def softmax(scores, lo):
        diagonal = jnp.where(allowed, scores[:, lo:], NEGATIVE)
        scores = jnp.concatenate([scores[:, :lo], diagonal], axis=1) if lo else diagonal
        exponent = jnp.exp(scores - jnp.max(scores, axis=-1, keepdims=True))
        return exponent * (1.0 / jnp.sum(exponent, axis=-1, keepdims=True))

    for block in reversed(range(blocks)):
        lo = block * rows
        hi = lo + rows
        q = q_ref[lo:hi, :].astype(jnp.float32) * scaling
        zero = jnp.zeros_like(q)
        stacked = jnp.concatenate([jnp.where(first, q, zero), jnp.where(first, zero, q)], axis=0)
        keys = k_ref[:hi, :]
        values = v_ref[:hi, :]
        scores = dot_nt(stacked.astype(jnp.bfloat16), keys)
        p1 = softmax(scores[:rows], lo)
        p2 = softmax(scores[rows:], lo)
        w2 = lam * p2
        weights = (p1 - w2).astype(jnp.bfloat16)
        mixed = dot(weights, values)
        inverse = lax.rsqrt(jnp.mean(mixed * mixed, axis=-1, keepdims=True) + EPS)
        normed = mixed * inverse
        cotan = g_ref[lo:hi, :].astype(jnp.float32)
        grad_mixed = inverse * (cotan - normed * jnp.mean(cotan * normed, axis=-1, keepdims=True))
        grad_weights = dot_nt(grad_mixed.astype(jnp.bfloat16), values)
        value_part = dot(grad_mixed.T.astype(jnp.bfloat16), weights)
        t1 = jnp.sum(grad_weights * p1, axis=-1, keepdims=True)
        t2 = jnp.sum(grad_weights * p2, axis=-1, keepdims=True)
        grad_lambda = grad_lambda - t2
        ds = jnp.concatenate(
            [
                (p1 * (grad_weights - t1)).astype(jnp.bfloat16),
                (w2 * (t2 - grad_weights)).astype(jnp.bfloat16),
            ],
            axis=0,
        )
        dq = dot(ds, keys)
        gq_ref[lo:hi, :] = (jnp.where(first, dq[:rows], dq[rows:]) * scaling).astype(jnp.bfloat16)
        key_part = dot(stacked.T.astype(jnp.bfloat16), ds)
        if block == blocks - 1:
            dv_acc[...] = value_part
            dk_acc[...] = key_part
        else:
            dv_acc[:, :hi] += value_part
            dk_acc[:, :hi] += key_part
    gk_ref[...] = dk_acc[...].T.astype(jnp.bfloat16)
    v_ref[...] = dv_acc[...].T.astype(jnp.bfloat16)
    gown_ref[...] = v_ref[own_rows, :]
    gother_ref[...] = v_ref[other_rows, :]
    gl_ref[...] = jnp.broadcast_to(jnp.sum(grad_lambda).reshape(1, 1), gl_ref.shape)


def head_backward(queries, keys, own, other, cotangent, lambdas, place, head):
    seq_length = queries.shape[0]
    span, width = own.shape
    block = pl.BlockSpec((seq_length, width), lambda i: (0, head))
    whole = pl.BlockSpec((seq_length, width), lambda i: (0, 0))
    part = pl.BlockSpec((span, width), lambda i: (0, 0))
    smem = pl.BlockSpec(memory_space=pltpu.SMEM)
    grads = jax.ShapeDtypeStruct((seq_length, width), jnp.bfloat16)
    halves = jax.ShapeDtypeStruct((span, width), jnp.bfloat16)
    return pl.pallas_call(
        functools.partial(attention_kernel, head=head),
        grid=(1,),
        in_specs=[smem, smem, block, block, part, part, block],
        out_specs=[whole, whole, part, part, pl.BlockSpec((8, 128), lambda i: (0, 0))],
        out_shape=[grads, grads, halves, halves, jax.ShapeDtypeStruct((8, 128), jnp.float32)],
        scratch_shapes=[
            pltpu.VMEM((width, seq_length), jnp.float32),
            pltpu.VMEM((width, seq_length), jnp.float32),
            pltpu.VMEM((seq_length, width), jnp.bfloat16),
        ],
        compiler_params=pltpu.CompilerParams(dimension_semantics=("arbitrary",)),
        cost_estimate=pl.CostEstimate(
            flops=20 * seq_length * seq_length * width,
            bytes_accessed=14 * seq_length * width,
            transcendentals=2 * seq_length * seq_length,
        ),
    )(lambdas, place, queries, keys, own, other, cotangent)


def rounds(axis):
    size = lax.axis_size(axis)
    mine = lax.axis_index(axis)
    for k in range(1, size):
        if size & (size - 1) == 0:
            yield [i ^ k for i in range(size)], mine ^ k, mine ^ k
        else:
            yield [(i + k) % size for i in range(size)], (mine + k) % size, (mine - k) % size


def send(x, axis, target):
    return lax.ppermute(x, axis, list(enumerate(target)))


def gathered(x, axis):
    pieces = [(lax.axis_index(axis), x)]
    for target, _, source in rounds(axis):
        pieces.append((source, send(x, axis, target)))
    return pieces


def scattered_sum(x, axis):
    total = lax.dynamic_index_in_dim(x, lax.axis_index(axis), 0, keepdims=False)
    total = total.astype(jnp.float32)
    for target, to, _ in rounds(axis):
        block = lax.dynamic_index_in_dim(x, to, 0, keepdims=False)
        total = total + send(block, axis, target).astype(jnp.float32)
    return total.astype(x.dtype)


def tied(*values):
    return lax.optimization_barrier(values)


def body(tokens, cotangent, value_weight, query_heads, key_heads, lambdas):
    groups = lax.axis_size("g")
    pair = lax.axis_size("p")
    chips = lax.axis_size("x")
    cores = lax.axis_size("c")
    local_tokens = tokens[0]
    block_tokens, model_width = local_tokens.shape
    row_count, features = value_weight.shape
    head_features = features // (pair * groups)
    group_features = pair * head_features
    seq_length = query_heads.shape[1]
    heads = lambdas.shape[0]
    width = head_features // heads
    place = lax.axis_index("p")
    swap = [1, 0]

    mine = lax.all_to_all(
        value_weight.reshape(row_count, pair, groups, head_features)
        .transpose(2, 0, 1, 3)
        .reshape(groups, row_count, group_features),
        "g",
        split_axis=0,
        concat_axis=0,
        tiled=True,
    )
    mine, local_tokens = tied(mine, local_tokens)
    columns = jnp.zeros((pair, groups, chips, cores, row_count, group_features), mine.dtype)
    p_pieces = gathered(mine, "p")
    far, cotangent = tied(p_pieces[1][1], cotangent)
    p_pieces[1] = (p_pieces[1][0], far)
    for p_index, p_piece in p_pieces:
        for x_index, x_piece in gathered(p_piece, "x"):
            for c_index, piece in gathered(x_piece, "c"):
                columns = lax.dynamic_update_slice(
                    columns, piece[None, :, None, None], (p_index, 0, x_index, c_index, 0, 0)
                )
    columns = columns.reshape(model_width, group_features)

    some_tokens = jnp.zeros((groups, block_tokens, model_width), tokens.dtype)
    for index, piece in gathered(local_tokens, "g"):
        some_tokens = lax.dynamic_update_slice(some_tokens, piece[None], (index, 0, 0))
    some_tokens = some_tokens.reshape(groups * block_tokens, model_width)

    cotan_heads = lax.all_to_all(
        cotangent[0], ("p", "g"), split_axis=1, concat_axis=0, tiled=True
    )
    some_values = dot(some_tokens, columns).astype(jnp.bfloat16)
    flat = (seq_length, head_features)
    queries = query_heads.reshape(flat)
    keys = key_heads.reshape(flat)
    own_values = lax.dynamic_slice_in_dim(some_values, place * head_features, head_features, 1)
    other_values = lax.dynamic_slice_in_dim(
        some_values, (1 - place) * head_features, head_features, 1
    )
    arrived = [
        send(other_values[:, h * width : (h + 1) * width], "p", swap) for h in range(heads)
    ]
    grad_queries, grad_keys, own_grads, other_grads, grad_lambda = [], [], [], [], []
    for h in range(heads):
        gq, gk, gown, gother, gl = head_backward(
            queries,
            keys,
            own_values[:, h * width : (h + 1) * width],
            arrived[h],
            cotan_heads,
            lambdas,
            place.reshape(1).astype(jnp.int32),
            h,
        )
        grad_queries.append(gq)
        grad_keys.append(gk)
        own_grads.append(gown)
        other_grads.append(send(gother, "p", swap))
        grad_lambda.append(gl[0, 0])
    own_grads = jnp.concatenate(own_grads, axis=1)
    other_grads = jnp.concatenate(other_grads, axis=1)
    grad_values = jnp.where(
        place == 0,
        jnp.concatenate([own_grads, other_grads], axis=1),
        jnp.concatenate([other_grads, own_grads], axis=1),
    )

    parts = dot_nt(grad_values, columns).astype(jnp.bfloat16)
    parts, some_tokens = tied(parts, some_tokens)
    parts = lax.all_to_all(
        parts.reshape(groups, block_tokens, model_width), "g", split_axis=0, concat_axis=0, tiled=True
    )
    grad_tokens = jnp.sum(parts.astype(jnp.float32), axis=0).astype(jnp.bfloat16)

    grad_lambda = jnp.stack(grad_lambda)
    lambda_grad = grad_lambda
    for target, _, _ in rounds(("x", "c")):
        lambda_grad = lambda_grad + send(grad_lambda, ("x", "c"), target)

    term = lax.dot_general(
        some_tokens, grad_values, (((0,), (0,)), ((), ())), preferred_element_type=jnp.float32
    ).astype(jnp.bfloat16)
    term = term.reshape(pair, groups, chips, cores, row_count, group_features)
    term = scattered_sum(term.transpose(3, 2, 0, 1, 4, 5), "c")
    chunks = []
    for start in range(0, group_features, head_features):
        chunk = term[..., start : start + head_features]
        chunks.append(scattered_sum(scattered_sum(chunk, "x"), "p"))
    term = jnp.stack(chunks, axis=2)
    term, lambda_grad = tied(term, lambda_grad)

    grad_weight = lax.all_to_all(term, "g", split_axis=0, concat_axis=0, tiled=True)
    grad_weight = grad_weight.reshape(groups, row_count, pair, head_features)
    grad_weight = grad_weight.transpose(1, 2, 0, 3).reshape(row_count, features)
    return (
        jnp.stack(grad_queries, axis=1)[None],
        jnp.stack(grad_keys, axis=1)[None],
        grad_tokens[None],
        grad_weight.astype(jnp.float32),
        lambda_grad,
    )


def solution(mesh):
    sp_count = mesh.shape["sp"]
    dp_count = mesh.shape["dp"]
    pair = cores = 2
    inner = Mesh(
        mesh.devices.reshape(pair, sp_count // pair, dp_count // cores, cores),
        ("p", "g", "x", "c"),
    )
    sp = ("p", "g")
    dp = ("x", "c")
    token_spec = P(dp, sp, None)
    head_spec = P(dp, None, sp, None)
    weight_spec = P(sp + dp, None)
    return jax.shard_map(
        body,
        mesh=inner,
        in_specs=(token_spec, token_spec, weight_spec, head_spec, head_spec, P(sp)),
        out_specs=(head_spec, head_spec, token_spec, weight_spec, P(sp)),
        check_vma=False,
    )
```

```python
import functools

import jax
import jax.numpy as jnp
from jax import lax
from jax.experimental import pallas as pl
from jax.experimental.pallas import tpu as pltpu
from jax.sharding import Mesh
from jax.sharding import PartitionSpec as P


QBLOCK = 256


EPS = 1e-06
NEGATIVE = -1e30

NT = (((1,), (1,)), ((), ()))


def dot(a, b):
    return jnp.dot(a, b, preferred_element_type=jnp.float32)


def dot_nt(a, b):
    return lax.dot_general(a, b, NT, preferred_element_type=jnp.float32)


def attention_kernel(
    lambda_ref,
    place_ref,
    q_ref,
    k_ref,
    own_ref,
    other_ref,
    g_ref,
    gq_ref,
    gk_ref,
    gown_ref,
    gother_ref,
    gl_ref,
    dk_acc,
    dv_acc,
    v_ref,
    *,
    head,
):
    seq_length, width = q_ref.shape
    span = own_ref.shape[0]
    own_rows = pl.ds(pl.multiple_of(place_ref[0] * span, span), span)
    other_rows = pl.ds(pl.multiple_of((1 - place_ref[0]) * span, span), span)
    v_ref[own_rows, :] = own_ref[...]
    v_ref[other_rows, :] = other_ref[...]
    half = width // 2
    scaling = half ** (-0.5)
    rows = min(QBLOCK, seq_length)
    blocks = seq_length // rows
    lam = lambda_ref[head]
    first = lax.broadcasted_iota(jnp.int32, (rows, width), 1) < half
    allowed = lax.broadcasted_iota(jnp.int32, (rows, rows), 0) >= lax.broadcasted_iota(
        jnp.int32, (rows, rows), 1
    )
    grad_lambda = jnp.zeros((rows, 1), jnp.float32)

    def softmax(scores, lo):
        diagonal = jnp.where(allowed, scores[:, lo:], NEGATIVE)
        scores = jnp.concatenate([scores[:, :lo], diagonal], axis=1) if lo else diagonal
        exponent = jnp.exp(scores - jnp.max(scores, axis=-1, keepdims=True))
        return exponent * (1.0 / jnp.sum(exponent, axis=-1, keepdims=True))

    for block in reversed(range(blocks)):
        lo = block * rows
        hi = lo + rows
        q = q_ref[lo:hi, :].astype(jnp.float32) * scaling
        zero = jnp.zeros_like(q)
        stacked = jnp.concatenate([jnp.where(first, q, zero), jnp.where(first, zero, q)], axis=0)
        keys = k_ref[:hi, :]
        values = v_ref[:hi, :]
        scores = dot_nt(stacked.astype(jnp.bfloat16), keys)
        p1 = softmax(scores[:rows], lo)
        p2 = softmax(scores[rows:], lo)
        w2 = lam * p2
        weights = (p1 - w2).astype(jnp.bfloat16)
        mixed = dot(weights, values)
        inverse = lax.rsqrt(jnp.mean(mixed * mixed, axis=-1, keepdims=True) + EPS)
        normed = mixed * inverse
        cotan = g_ref[lo:hi, :].astype(jnp.float32)
        grad_mixed = inverse * (cotan - normed * jnp.mean(cotan * normed, axis=-1, keepdims=True))
        grad_weights = dot_nt(grad_mixed.astype(jnp.bfloat16), values)
        value_part = dot(grad_mixed.T.astype(jnp.bfloat16), weights)
        t1 = jnp.sum(grad_weights * p1, axis=-1, keepdims=True)
        t2 = jnp.sum(grad_weights * p2, axis=-1, keepdims=True)
        grad_lambda = grad_lambda - t2
        ds = jnp.concatenate(
            [
                (p1 * (grad_weights - t1)).astype(jnp.bfloat16),
                (w2 * (t2 - grad_weights)).astype(jnp.bfloat16),
            ],
            axis=0,
        )
        dq = dot(ds, keys)
        gq_ref[lo:hi, :] = (jnp.where(first, dq[:rows], dq[rows:]) * scaling).astype(jnp.bfloat16)
        key_part = dot(stacked.T.astype(jnp.bfloat16), ds)
        if block == blocks - 1:
            dv_acc[...] = value_part
            dk_acc[...] = key_part
        else:
            dv_acc[:, :hi] += value_part
            dk_acc[:, :hi] += key_part
    gk_ref[...] = dk_acc[...].T.astype(jnp.bfloat16)
    v_ref[...] = dv_acc[...].T.astype(jnp.bfloat16)
    gown_ref[...] = v_ref[own_rows, :]
    gother_ref[...] = v_ref[other_rows, :]
    gl_ref[...] = jnp.broadcast_to(jnp.sum(grad_lambda).reshape(1, 1), gl_ref.shape)


def head_backward(queries, keys, own, other, cotangent, lambdas, place, head):
    seq_length = queries.shape[0]
    span, width = own.shape
    block = pl.BlockSpec((seq_length, width), lambda i: (0, head))
    whole = pl.BlockSpec((seq_length, width), lambda i: (0, 0))
    part = pl.BlockSpec((span, width), lambda i: (0, 0))
    smem = pl.BlockSpec(memory_space=pltpu.SMEM)
    grads = jax.ShapeDtypeStruct((seq_length, width), jnp.bfloat16)
    halves = jax.ShapeDtypeStruct((span, width), jnp.bfloat16)
    return pl.pallas_call(
        functools.partial(attention_kernel, head=head),
        grid=(1,),
        in_specs=[smem, smem, block, block, part, part, block],
        out_specs=[whole, whole, part, part, pl.BlockSpec((8, 128), lambda i: (0, 0))],
        out_shape=[grads, grads, halves, halves, jax.ShapeDtypeStruct((8, 128), jnp.float32)],
        scratch_shapes=[
            pltpu.VMEM((width, seq_length), jnp.float32),
            pltpu.VMEM((width, seq_length), jnp.float32),
            pltpu.VMEM((seq_length, width), jnp.bfloat16),
        ],
        compiler_params=pltpu.CompilerParams(dimension_semantics=("arbitrary",)),
        cost_estimate=pl.CostEstimate(
            flops=20 * seq_length * seq_length * width,
            bytes_accessed=14 * seq_length * width,
            transcendentals=2 * seq_length * seq_length,
        ),
    )(lambdas, place, queries, keys, own, other, cotangent)


def value_kernel(place_ref, *refs, token_count, weight_count, stride):
    token_refs = refs[:token_count]
    weight_refs = refs[token_count : token_count + weight_count]
    tokens_ref, columns_ref, own_ref, other_ref = refs[token_count + weight_count :]
    block = token_refs[0].shape[0]
    for i, ref in enumerate(token_refs):
        start = pl.multiple_of(place_ref[1 + i] * block, block)
        tokens_ref[pl.ds(start, block), :] = ref[...]
    groups, rows, _ = weight_refs[0].shape
    for i, ref in enumerate(weight_refs):
        for g in range(groups):
            start = pl.multiple_of(
                (place_ref[1 + token_count + i] + g * stride) * rows, rows
            )
            columns_ref[pl.ds(start, rows), :] = ref[g]
    half = own_ref.shape[1]
    first = place_ref[0] == 0
    for i in range(token_count):
        span = slice(i * block, (i + 1) * block)
        low = dot(tokens_ref[span, :], columns_ref[:, :half]).astype(jnp.bfloat16)
        high = dot(tokens_ref[span, :], columns_ref[:, half:]).astype(jnp.bfloat16)

        @pl.when(first)
        def _():
            own_ref[span, :] = low
            other_ref[span, :] = high

        @pl.when(jnp.logical_not(first))
        def _():
            own_ref[span, :] = high
            other_ref[span, :] = low


def value_product(tokens, token_places, weights, weight_places, place, stride):
    block, model_width = tokens[0].shape
    columns = weights[0].shape[2]
    rows = len(tokens) * block
    vmem = pl.BlockSpec(memory_space=pltpu.VMEM)
    places = jnp.stack([place, *token_places, *weight_places]).astype(jnp.int32)
    return pl.pallas_call(
        functools.partial(
            value_kernel, token_count=len(tokens), weight_count=len(weights), stride=stride
        ),
        in_specs=[pl.BlockSpec(memory_space=pltpu.SMEM)] + [vmem] * (len(tokens) + len(weights)),
        out_specs=[vmem] * 4,
        out_shape=[
            jax.ShapeDtypeStruct((rows, model_width), jnp.bfloat16),
            jax.ShapeDtypeStruct((model_width, columns), jnp.bfloat16),
            jax.ShapeDtypeStruct((rows, columns // 2), jnp.bfloat16),
            jax.ShapeDtypeStruct((rows, columns // 2), jnp.bfloat16),
        ],
        cost_estimate=pl.CostEstimate(
            flops=2 * rows * model_width * columns,
            bytes_accessed=4 * (rows + columns) * model_width,
            transcendentals=0,
        ),
    )(places, *tokens, *weights)


def rounds(axis):
    size = lax.axis_size(axis)
    mine = lax.axis_index(axis)
    for k in range(1, size):
        if size & (size - 1) == 0:
            yield [i ^ k for i in range(size)], mine ^ k, mine ^ k
        else:
            yield [(i + k) % size for i in range(size)], (mine + k) % size, (mine - k) % size


def send(x, axis, target):
    return lax.ppermute(x, axis, list(enumerate(target)))


def gathered(x, axis):
    pieces = [(lax.axis_index(axis), x)]
    for target, _, source in rounds(axis):
        pieces.append((source, send(x, axis, target)))
    return pieces


def scattered_sum(x, axis):
    total = lax.dynamic_index_in_dim(x, lax.axis_index(axis), 0, keepdims=False)
    total = total.astype(jnp.float32)
    for target, to, _ in rounds(axis):
        block = lax.dynamic_index_in_dim(x, to, 0, keepdims=False)
        total = total + send(block, axis, target).astype(jnp.float32)
    return total.astype(x.dtype)


def exchanged(x, axis):
    out = lax.dynamic_update_slice_in_dim(
        x,
        lax.dynamic_slice_in_dim(x, lax.axis_index(axis), 1, 0),
        lax.axis_index(axis),
        0,
    )
    for target, to, source in rounds(axis):
        block = lax.dynamic_slice_in_dim(x, to, 1, 0)
        out = lax.dynamic_update_slice_in_dim(out, send(block, axis, target), source, 0)
    return out


def tied(*values):
    return lax.optimization_barrier(values)


def body(tokens, cotangent, value_weight, query_heads, key_heads, lambdas):
    groups = lax.axis_size("g")
    pair = lax.axis_size("p")
    chips = lax.axis_size("x")
    cores = lax.axis_size("c")
    local_tokens = tokens[0]
    block_tokens, model_width = local_tokens.shape
    row_count, features = value_weight.shape
    head_features = features // (pair * groups)
    group_features = pair * head_features
    seq_length = query_heads.shape[1]
    heads = lambdas.shape[0]
    width = head_features // heads
    place = lax.axis_index("p")
    swap = [1, 0]

    mine = exchanged(
        value_weight.reshape(row_count, pair, groups, head_features)
        .transpose(2, 0, 1, 3)
        .reshape(groups, row_count, group_features),
        "g",
    )
    mine, local_tokens = tied(mine, local_tokens)
    p_pieces = gathered(mine, "p")
    far, cotangent = tied(p_pieces[1][1], cotangent)
    p_pieces[1] = (p_pieces[1][0], far)
    weight_pieces, weight_places = [], []
    for p_index, p_piece in p_pieces:
        x_pieces = gathered(p_piece, "x")
        for x_index, x_piece in x_pieces:
            for c_index, piece in gathered(x_piece, "c"):
                weight_pieces.append(piece)
                weight_places.append((p_index * groups * chips + x_index) * cores + c_index)

    token_places, token_pieces = zip(*gathered(local_tokens, "g"))

    cotan_heads = lax.all_to_all(
        cotangent[0], ("p", "g"), split_axis=1, concat_axis=0, tiled=True
    )
    some_tokens, columns, own_values, other_values = value_product(
        token_pieces, token_places, weight_pieces, weight_places, place, chips * cores
    )
    flat = (seq_length, head_features)
    queries = query_heads.reshape(flat)
    keys = key_heads.reshape(flat)
    arrived = [
        send(other_values[:, h * width : (h + 1) * width], "p", swap) for h in range(heads)
    ]
    grad_queries, grad_keys, own_grads, other_grads, grad_lambda = [], [], [], [], []
    for h in range(heads):
        gq, gk, gown, gother, gl = head_backward(
            queries,
            keys,
            own_values[:, h * width : (h + 1) * width],
            arrived[h],
            cotan_heads,
            lambdas,
            place.reshape(1).astype(jnp.int32),
            h,
        )
        grad_queries.append(gq)
        grad_keys.append(gk)
        own_grads.append(gown)
        other_grads.append(send(gother, "p", swap))
        grad_lambda.append(gl[0, 0])
    own_grads = jnp.concatenate(own_grads, axis=1)
    other_grads = jnp.concatenate(other_grads, axis=1)
    grad_values = jnp.where(
        place == 0,
        jnp.concatenate([own_grads, other_grads], axis=1),
        jnp.concatenate([other_grads, own_grads], axis=1),
    )

    parts = dot_nt(grad_values, columns).astype(jnp.bfloat16)
    parts = parts.reshape(groups, block_tokens, model_width)
    blocks = [lax.dynamic_index_in_dim(parts, lax.axis_index("g"), 0, keepdims=False)]
    targets = []
    for target, to, _ in rounds("g"):
        targets.append(target)
        blocks.append(lax.dynamic_index_in_dim(parts, to, 0, keepdims=False))
    *blocks, some_tokens = tied(*blocks, some_tokens)
    own_part = blocks[0]
    parts = [send(block, "g", target) for target, block in zip(targets, blocks[1:])]

    term = lax.dot_general(
        some_tokens, grad_values, (((0,), (0,)), ((), ())), preferred_element_type=jnp.float32
    ).astype(jnp.bfloat16)
    term = term.reshape(pair, groups, chips, cores, row_count, group_features)
    term = scattered_sum(term.transpose(3, 2, 0, 1, 4, 5), "c")
    chunks = [
        scattered_sum(term[..., start : start + head_features], "x")
        for start in range(0, group_features, head_features)
    ]
    grad_lambda, chunks[-1] = tied(jnp.stack(grad_lambda), chunks[-1])
    lambda_grad = grad_lambda
    for target, _, _ in rounds(("x", "c")):
        lambda_grad = lambda_grad + send(grad_lambda, ("x", "c"), target)
    term = jnp.concatenate([scattered_sum(chunk, "p") for chunk in chunks], axis=-1)

    grad_weight = exchanged(term, "g")
    grad_weight = grad_weight.reshape(groups, row_count, pair, head_features)
    grad_weight = grad_weight.transpose(1, 2, 0, 3).reshape(row_count, features)
    grad_weight = grad_weight.astype(jnp.float32)
    grad_weight, *parts = tied(grad_weight, *parts)
    grad_tokens = own_part.astype(jnp.float32)
    for part in parts:
        grad_tokens = grad_tokens + part.astype(jnp.float32)
    grad_tokens = grad_tokens.astype(jnp.bfloat16)
    return (
        jnp.stack(grad_queries, axis=1)[None],
        jnp.stack(grad_keys, axis=1)[None],
        grad_tokens[None],
        grad_weight,
        lambda_grad,
    )


def solution(mesh):
    sp_count = mesh.shape["sp"]
    dp_count = mesh.shape["dp"]
    pair = cores = 2
    inner = Mesh(
        mesh.devices.reshape(pair, sp_count // pair, dp_count // cores, cores),
        ("p", "g", "x", "c"),
    )
    sp = ("p", "g")
    dp = ("x", "c")
    token_spec = P(dp, sp, None)
    head_spec = P(dp, None, sp, None)
    weight_spec = P(sp + dp, None)

    return jax.shard_map(
        body,
        mesh=inner,
        in_specs=(token_spec, token_spec, weight_spec, head_spec, head_spec, P(sp)),
        out_specs=(head_spec, head_spec, token_spec, weight_spec, P(sp)),
        check_vma=False,
    )
```
